32 devices in a mesh: sp: 16 (over z, y, core), tp: 2 (over x).
Axes of the slice: x: 2, y: 2, z: 4, core: 2. Of those that a mesh axis runs over, the one named last changes fastest.
Arguments:
- resid: bfloat16 [8192, 2048], P(('sp', 'tp')), may hold values from -3 to 3
- queries: bfloat16 [8192, 1024], P('sp', 'tp'), may hold values from -6 to 6
- keys: bfloat16 [8192, 512], P('sp', 'tp'), may hold values from -6 to 6
- values: bfloat16 [8192, 512], P('sp', 'tp'), may hold values from -6 to 6
- documents: int32 [8192], P('sp'), may hold values from 0 to 7, never falling along the last dimension, each value on 1 to 2048 neighbouring positions
- sinks: float32 [16], P('tp'), may hold values from 0 to 5
- out_proj: bfloat16 [1024, 2048], replicated, may hold values from -0.75 to 0.75
- norm_gain: float32 [2048], replicated, may hold values from 0.1 to 1.9
- gate_proj: bfloat16 [2048, 5632], P('sp', 'tp'), may hold values from -0.125 to 0.125
- up_proj: bfloat16 [2048, 5632], P('sp', 'tp'), may hold values from -0.125 to 0.125
- down_proj: bfloat16 [5632, 2048], P('tp', 'sp'), may hold values from -0.078125 to 0.078125
Outputs:
- mixed: bfloat16 [8192, 2048], P(('sp', 'tp'))
The draws below stay inside these ranges and needn't reach their ends.
Inputs may be any that keep to these rules, and one draw needn't show every extreme that they name: `documents`: document numbers never fall along the sequence; each document holds at most 2048 positions.
All inputs are finite; a program needn't handle non-finite values.
Results may differ from the reference program's by a relative error of at most 0.0095.
Values may be sent and summed in bfloat16 or wider, within the bound.
A program may use at most 128 MiB of HBM per device.

```python
import math
import jax
import jax.numpy as jnp
import numpy as np
from jax import lax

D = 2048
FF = 5632
HEADS = 16
KV_HEADS = 8
HD = 64
WINDOW = 128
TOK_DEV = 512
TOKENS = 8192
DOCS = 8
N_TP = 2


def draw_pair(key):
    base = jax.random.fold_in(key, 17)
    first, second = jax.random.split(base, 2)
    queries = jnp.clip(jax.random.normal(first, (TOKENS, HEADS * HD), jnp.float32), -6.0, 6.0)
    keys = jnp.clip(jax.random.normal(second, (TOKENS, KV_HEADS * HD), jnp.float32), -6.0, 6.0)
    return (queries, keys)


def draw_queries(key, part):
    return draw_pair(key)[0].astype(jnp.bfloat16)


def draw_keys(key, part):
    return draw_pair(key)[1].astype(jnp.bfloat16)


def block_scale(stream_key, dims, cuts, low, top_value):
    loudness, own = 1.0, jax.random.fold_in(stream_key, 6)
    for position, shards_of in cuts:
        steps = jnp.exp(jax.random.uniform(jax.random.fold_in(own, position), (shards_of,), jnp.float32, low / len(cuts), top_value / len(cuts)))
        loudness = loudness * jnp.repeat(steps, dims[position] // shards_of).reshape([-1 if axis == position else 1 for axis in range(len(dims))])
    return loudness


def length_profile(amount, total, limit, skew):
    weights = [(1 << 20) // math.isqrt(rank ** skew) + 1 for rank in range(2, amount + 1)]
    surplus, given = total - limit - (amount - 1), [1] * (amount - 1)
    while surplus > 0:
        candidates = [i for i in range(amount - 1) if given[i] < limit]
        pool, remaining = sum([weights[i] for i in candidates]), surplus
        for i in candidates:
            addition = min(limit - given[i], max(1, remaining * weights[i] // pool), surplus)
            given[i] = given[i] + addition
            surplus = surplus - addition
    return np.array([limit] + given)


def uneven_parts(key, count, total, most, skew):
    if count == 2:
        one = jax.random.randint(key, (), max(1, total - most), min(most, total - 1) + 1)
        return jnp.stack([one, total - one])
    tallies = jnp.asarray(length_profile(count, total, most, skew), jnp.int32)
    twos = (count - 1) // 2
    giver, receiver = tallies[1:1 + 2 * twos:2], tallies[2:2 + 2 * twos:2]
    slack = jnp.minimum(giver - 1, most - receiver)
    shifted = jax.random.randint(jax.random.fold_in(key, 1), (twos,), 0, 1 << 20) % (slack + 1)
    tallies = tallies.at[1:1 + 2 * twos:2].set(giver - shifted).at[2:2 + 2 * twos:2].set(receiver + shifted)
    return tallies[jax.random.permutation(jax.random.fold_in(key, 2), count)]


def noise(key, shape, deviation, limit, cuts=(), held_as=jnp.bfloat16):
    loudness = block_scale(key, shape, cuts, -0.22, 0.18) if cuts else 1.0
    entries = jax.random.normal(key, shape, jnp.float32) * deviation * loudness
    return jnp.minimum(jnp.maximum(entries, -limit), limit).astype(held_as)


def setup_inputs(seed: int = 0) -> dict:
    splits = jax.random.split(jax.random.key(seed), 12)
    resid = noise(splits[0], (TOKENS, D), 0.5, 3.0, ((0, 32),))
    queries = draw_queries(jax.random.fold_in(splits[11], 71), 0)
    keys = draw_keys(jax.random.fold_in(splits[11], 71), 0)
    values = noise(splits[3], (TOKENS, KV_HEADS * HD), 1.0, 6.0, ((0, 16), (1, 2)))
    documents = jnp.searchsorted(jnp.cumsum(uneven_parts(splits[4], DOCS, TOKENS, 4 * TOK_DEV, 0)), jnp.arange(TOKENS), side="right").astype(jnp.int32)
    sinks = jnp.clip(5.0 * jax.random.uniform(splits[5], (HEADS,), jnp.float32) ** block_scale(splits[5], (HEADS,), ((0, 2),), -0.2, 0.2), 0.0, 5.0)
    out_proj = noise(splits[6], (HEADS * HD, D), HD ** -0.5, 0.75)
    norm_gain = jnp.clip(1.0 + 0.18 * jax.random.normal(splits[7], (D,), jnp.float32), 0.1, 1.9)
    gate_proj = noise(splits[8], (D, FF), D ** -0.5, 0.125, ((0, 16), (1, 2)))
    up_proj = noise(splits[9], (D, FF), D ** -0.5, 0.125, ((0, 16), (1, 2)))
    down_proj = noise(splits[10], (FF, D), FF ** -0.5, 0.078125, ((0, 2), (1, 16)))
    return {"resid": resid, "queries": queries, "keys": keys, "values": values, "documents": documents, "sinks": sinks, "out_proj": out_proj, "norm_gain": norm_gain, "gate_proj": gate_proj, "up_proj": up_proj, "down_proj": down_proj}


def band_attend(queries, keys, values, documents, sinks):
    rows = queries.shape[0]
    kv_heads = keys.shape[1] // HD
    group = queries.shape[1] // HD // kv_heads
    blocks = rows // WINDOW
    zero_keys = jnp.zeros((WINDOW, keys.shape[1]), jnp.float32)
    ext_keys = jnp.concatenate([zero_keys, keys.astype(jnp.float32)], axis=0).reshape(blocks + 1, WINDOW, kv_heads, HD)
    ext_values = jnp.concatenate([zero_keys, values.astype(jnp.float32)], axis=0).reshape(blocks + 1, WINDOW, kv_heads, HD)
    ext_docs = jnp.concatenate([jnp.zeros((WINDOW,), jnp.int32), documents.astype(jnp.int32)], axis=0).reshape(blocks + 1, WINDOW)
    band_keys = jnp.concatenate([ext_keys[:-1], ext_keys[1:]], axis=1)
    band_values = jnp.concatenate([ext_values[:-1], ext_values[1:]], axis=1)
    band_docs = jnp.concatenate([ext_docs[:-1], ext_docs[1:]], axis=1)
    query_docs = documents.reshape(blocks, WINDOW)
    distance = jnp.arange(WINDOW)[:, None] + WINDOW - jnp.arange(2 * WINDOW)[None, :]
    key_pos = jnp.arange(blocks)[:, None] * WINDOW + jnp.arange(2 * WINDOW)[None, :] - WINDOW
    visible = ((distance >= 0) & (distance < WINDOW))[None] & (key_pos >= 0)[:, None, :] & (band_docs[:, None, :] == query_docs[:, :, None])
    query_blocks = queries.astype(jnp.float32).reshape(blocks, WINDOW, kv_heads, group, HD)
    scores = jnp.einsum('nikgd,njkd->nkgij', query_blocks, band_keys) * HD ** (-0.5)
    scores = jnp.where(visible[:, None, None], scores, -jnp.inf)
    sink_logit = sinks.astype(jnp.float32).reshape(kv_heads, group)[None, :, :, None, None]
    row_top = jnp.maximum(lax.optimization_barrier(jnp.max(scores, axis=-1, keepdims=True)), sink_logit)
    raw_weights = jnp.exp(scores - row_top)
    totals = lax.optimization_barrier(jnp.sum(raw_weights, axis=-1, keepdims=True)) + jnp.exp(sink_logit - row_top)
    weights = (raw_weights / totals).astype(jnp.bfloat16).astype(jnp.float32)
    attended = jnp.einsum('nkgij,njkd->nikgd', weights, band_values)
    return attended.astype(jnp.bfloat16).reshape(rows, kv_heads * group * HD)

def reference(resid, queries, keys, values, documents, sinks, out_proj, norm_gain, gate_proj, up_proj, down_proj):
    group = HEADS // KV_HEADS
    pieces = []
    for head in range(KV_HEADS):
        pieces.append(band_attend(queries[:, head * group * HD:(head + 1) * group * HD], keys[:, head * HD:(head + 1) * HD], values[:, head * HD:(head + 1) * HD], documents, sinks[head * group:(head + 1) * group]))
    attended = jnp.concatenate(pieces, axis=1)
    mid_rows = resid.astype(jnp.float32) + jnp.dot(attended, out_proj, preferred_element_type=jnp.float32)
    scale = lax.rsqrt(lax.optimization_barrier(jnp.mean(mid_rows * mid_rows, axis=-1, keepdims=True)) + 1e-06)
    normed = (mid_rows * scale * norm_gain).astype(jnp.bfloat16)
    width = FF // N_TP

    def ffn_rows(row_block):
        gate_acts = jnp.dot(row_block, gate_proj, preferred_element_type=jnp.float32)
        up_acts = jnp.dot(row_block, up_proj, preferred_element_type=jnp.float32)
        hidden = (jax.nn.silu(gate_acts) * up_acts).astype(jnp.bfloat16)
        totals = jnp.zeros((row_block.shape[0], D), jnp.float32)
        for block in range(N_TP):
            partial_value = jnp.dot(hidden[:, block * width:(block + 1) * width], down_proj[block * width:(block + 1) * width], preferred_element_type=jnp.float32).astype(jnp.bfloat16)
            totals = totals + lax.optimization_barrier(partial_value).astype(jnp.float32)
        return totals
    summed = lax.map(ffn_rows, normed.reshape(TOKENS // TOK_DEV, TOK_DEV, D)).reshape(TOKENS, D)
    return (mid_rows + summed).astype(jnp.bfloat16)
```

```python
import jax
import jax.numpy as jnp
from jax import lax
from jax.sharding import PartitionSpec as P

HD = 64
WINDOW = 128
SHARE = 4


def passed_along(value, axis, steps):
    count = lax.axis_size(axis)
    first, last = (max(0, -steps), min(count, count - steps))
    return lax.ppermute(value, axis, [(source, source + steps) for source in range(first, last)])


def swapped(value, axis, mask):
    count = lax.axis_size(axis)
    return lax.ppermute(value, axis, [(source, source ^ mask) for source in range(count)])


def bits_of(count):
    return [1 << bit for bit in range(count.bit_length() - 1)]


def attend(queries, keys, values, documents, sinks):
    rows = queries.shape[0]
    kv_heads = keys.shape[1] // HD
    group = queries.shape[1] // HD // kv_heads
    blocks = rows // WINDOW
    key_value = jnp.concatenate([keys, values], axis=1)
    tail_pair, tail_docs = passed_along(
        (key_value[rows - WINDOW :], documents[rows - WINDOW :].astype(jnp.bfloat16)), "sp", 1
    )
    ext_pair = jnp.concatenate([tail_pair, key_value], axis=0).reshape(
        blocks + 1, WINDOW, 2 * kv_heads * HD
    )
    ext_docs = jnp.concatenate([tail_docs.astype(jnp.int32), documents], axis=0).reshape(
        blocks + 1, WINDOW
    )
    band = jnp.concatenate([ext_pair[:-1], ext_pair[1:]], axis=1)
    band_keys = band[:, :, : kv_heads * HD].reshape(blocks, 2 * WINDOW, kv_heads, HD)
    band_values = band[:, :, kv_heads * HD :].reshape(blocks, 2 * WINDOW, kv_heads, HD)
    band_docs = jnp.concatenate([ext_docs[:-1], ext_docs[1:]], axis=1)
    query_docs = documents.reshape(blocks, WINDOW)
    offset = lax.axis_index("sp") * rows
    distance = jnp.arange(WINDOW)[:, None] + WINDOW - jnp.arange(2 * WINDOW)[None, :]
    key_pos = (
        offset + jnp.arange(blocks)[:, None] * WINDOW + jnp.arange(2 * WINDOW)[None, :] - WINDOW
    )
    visible = (
        ((distance >= 0) & (distance < WINDOW))[None]
        & (key_pos >= 0)[:, None, :]
        & (band_docs[:, None, :] == query_docs[:, :, None])
    )
    query_blocks = queries.reshape(blocks, WINDOW, kv_heads, group, HD)
    scores = jnp.einsum(
        "nikgd,njkd->nkgij", query_blocks, band_keys, preferred_element_type=jnp.float32
    ) * HD ** (-0.5)
    scores = jnp.where(visible[:, None, None], scores, -jnp.inf)
    sink_logit = sinks.reshape(kv_heads, group)[None, :, :, None, None]
    row_top = jnp.maximum(jnp.max(scores, axis=-1, keepdims=True), sink_logit)
    raw_weights = jnp.exp(scores - row_top)
    totals = jnp.sum(raw_weights, axis=-1, keepdims=True) + jnp.exp(sink_logit - row_top)
    weights = (raw_weights / totals).astype(jnp.bfloat16)
    attended = jnp.einsum(
        "nkgij,njkd->nikgd", weights, band_values, preferred_element_type=jnp.float32
    )
    return attended.astype(jnp.bfloat16).reshape(rows, kv_heads * group * HD)


def norm_rows(mid_rows, norm_gain):
    scale = lax.rsqrt(jnp.mean(mid_rows * mid_rows, axis=-1, keepdims=True) + 1e-06)
    return (mid_rows * scale * norm_gain).astype(jnp.bfloat16)


def by_place(pieces, me):
    for bit in bits_of(len(pieces)):
        flip = (me & bit) != 0
        pieces = [jnp.where(flip, pieces[r ^ bit], pieces[r]) for r in range(len(pieces))]
    return pieces


def own_rows(attended):
    count = lax.axis_size("tp")
    me = lax.axis_index("tp")
    rows = attended.shape[0] // count
    pieces = []
    for mask in range(count):
        piece = lax.dynamic_slice_in_dim(attended, (me ^ mask) * rows, rows)
        pieces.append(swapped(piece, "tp", mask) if mask else piece)
    return jnp.concatenate(by_place(pieces, me), axis=1)


def regrouped(gate_proj, up_proj, down_proj):
    me = lax.axis_index("sp") % SHARE
    width = gate_proj.shape[1] // SHARE
    gate_up, down = [], []
    for mask in range(SHARE):
        start = (me ^ mask) * width
        piece = jnp.concatenate(
            [
                lax.dynamic_slice_in_dim(gate_proj, start, width, axis=1),
                lax.dynamic_slice_in_dim(up_proj, start, width, axis=1),
            ],
            axis=1,
        )
        gate_up.append(swapped(piece, "sp", mask) if mask else piece)
    for mask in range(SHARE):
        piece = lax.dynamic_slice_in_dim(down_proj, (me ^ mask) * width, width, axis=0)
        down.append(swapped(piece, "sp", mask) if mask else piece)
    return (
        jnp.concatenate(by_place(gate_up, me), axis=0),
        jnp.concatenate(by_place(down, me), axis=1),
    )


def spread(chunk):
    groups = lax.axis_size("sp") // SHARE
    if groups == 4:
        half = chunk.shape[0] // 2
        low = swapped(chunk, "sp", SHARE)
        wrap = swapped(chunk, "sp", 3 * SHARE)
        first = swapped(low[:half], "sp", 3 * SHARE)
        second = swapped(wrap[half:], "sp", SHARE)
        return [chunk, low, jnp.concatenate([first, second], axis=0), wrap]
    chunks = [chunk]
    for bit in bits_of(groups):
        chunks = chunks + [swapped(piece, "sp", SHARE * bit) for piece in chunks]
    return chunks


def gathered(rows, hops):
    for axis, mask in hops:
        rows = jnp.concatenate([rows, swapped(rows, axis, mask)], axis=0)
    return rows


def scattered(partial, hops):
    total = partial
    for axis, mask in reversed(hops):
        half = total.shape[0] // 2
        arrived = swapped(total[half:].astype(jnp.bfloat16), axis, mask)
        total = total[:half].astype(jnp.float32) + arrived.astype(jnp.float32)
    return total


def shards(
    resid,
    queries,
    keys,
    values,
    documents,
    sinks,
    out_proj,
    norm_gain,
    gate_proj,
    up_proj,
    down_proj,
):
    groups = lax.axis_size("sp") // SHARE
    group = lax.axis_index("sp") // SHARE
    gate_up, down = regrouped(gate_proj, up_proj, down_proj)
    gate_up = jnp.concatenate(spread(gate_up), axis=0)
    down = jnp.concatenate(spread(down), axis=1)
    units = down.shape[0]

    attended = attend(queries, keys, values, documents, sinks)
    mid_rows = resid.astype(jnp.float32) + jnp.dot(
        own_rows(attended), out_proj, preferred_element_type=jnp.float32
    )
    normed = norm_rows(mid_rows, norm_gain)
    rows, width = normed.shape
    block = width // groups
    normed = jnp.concatenate(
        [lax.dynamic_slice_in_dim(normed, (group ^ k) * block, block, axis=1) for k in range(groups)],
        axis=1,
    )
    x_hops = [("tp", bit) for bit in bits_of(lax.axis_size("tp"))]
    y_hops = [("sp", 2)]
    core_hops = [("sp", 1)]
    sums = []
    for stream, hops in enumerate((x_hops + y_hops + core_hops, y_hops + x_hops + core_hops)):
        part = normed[stream * rows // 2 : (stream + 1) * rows // 2]
        part = gathered(part, hops)
        acts = jnp.dot(part, gate_up, preferred_element_type=jnp.float32)
        hidden = (jax.nn.silu(acts[:, :units]) * acts[:, units:]).astype(jnp.bfloat16)
        partial = jnp.dot(hidden, down, preferred_element_type=jnp.float32).astype(jnp.bfloat16)
        sums.append(scattered(partial, hops))
    summed = jnp.concatenate(sums, axis=0)
    stack = jnp.stack([summed[:, k * block : (k + 1) * block] for k in range(groups)])
    summed = jnp.concatenate(
        [lax.dynamic_index_in_dim(stack, group ^ k, keepdims=False) for k in range(groups)], axis=1
    )
    return (mid_rows + summed).astype(jnp.bfloat16)


def solution(mesh):
    in_specs = (
        P(("sp", "tp"), None),
        P("sp", "tp"),
        P("sp", "tp"),
        P("sp", "tp"),
        P("sp"),
        P("tp"),
        P(),
        P(),
        P("sp", "tp"),
        P("sp", "tp"),
        P("tp", "sp"),
    )
    out_specs = P(("sp", "tp"), None)
    return jax.shard_map(shards, mesh=mesh, in_specs=in_specs, out_specs=out_specs, check_vma=False)
```
